32 devices in a mesh: grp: 1, ep: 16 (over z, y, x), tp: 2 (over core).
Axes of the slice: x: 2, y: 2, z: 4, core: 2. Of those that a mesh axis runs over, the one named last changes fastest.
Arguments:
- layer_input: bfloat16 [512, 2048], P(('grp', 'ep')), may hold values from -6 to 6
- ssm_state: float32 [2, 512, 32, 64], P(None, ('grp', 'ep'), 'tp'), may hold values from -4 to 4
- w_input: bfloat16 [2048, 512], P(None, 'tp'), may hold values from -0.125 to 0.125
- decay_rate: float32 [32, 64], P('tp'), may hold values from 0.05 to 2
- frequency: float32 [32, 64], P('tp'), may hold values from 0 to 20
- step_log: float32 [32], P('tp'), may hold values from -2.3 to 0
- input_map: float32 [2, 32, 64, 16], P(None, 'tp'), may hold values from -1 to 1
- output_map: float32 [2, 32, 16, 64], P(None, 'tp'), may hold values from -0.75 to 0.75
- skip_gain: float32 [32, 16], P('tp'), may hold values from -3 to 3
- glu_weight: bfloat16 [512, 512], replicated, may hold values from -0.25 to 0.25
- mix_out: bfloat16 [512, 2048], replicated, may hold values from -0.75 to 0.75
- norm_gain: float32 [2048], replicated, may hold values from 0.1 to 6, as said below
- norm_shift: float32 [2048], replicated, may hold values from -2 to 2
- route_ids: int32 [512, 6], P(('grp', 'ep')), may hold values from 0 to 15, all different within a row; in each aligned block of 32 rows (0 to 31, 32 to 63, ...) at most 24 rows name the same one
- route_weights: float32 [512, 6], P(('grp', 'ep')), may hold values from 0.1 to 1
- gate_expert: bfloat16 [16, 2048, 512], P('ep', None, 'tp'), may hold values from -0.125 to 0.125
- up_expert: bfloat16 [16, 2048, 512], P('ep', None, 'tp'), may hold values from -0.125 to 0.125
- down_expert: bfloat16 [16, 512, 2048], P('ep', 'tp'), may hold values from -0.25 to 0.25
- gate_shared: bfloat16 [2048, 512], P(None, 'tp'), may hold values from -0.125 to 0.125
- up_shared: bfloat16 [2048, 512], P(None, 'tp'), may hold values from -0.125 to 0.125
- down_shared: bfloat16 [512, 2048], P('tp'), may hold values from -0.25 to 0.25
- dense_in: bfloat16 [1024, 2048], P('ep'), may hold values from -0.125 to 0.125
- dense_out: bfloat16 [1024, 2048], P('ep', 'tp'), may hold values from -0.1875 to 0.1875
- branch_gate: bfloat16 [2048], replicated, may hold values from -0.125 to 0.125
- final_gain: float32 [2048], P('tp'), may hold values from 0.1 to 1.9
- final_shift: float32 [2048], P('tp'), may hold values from -2 to 2
Outputs:
- layer_output: bfloat16 [512, 2048], P(('grp', 'ep'), 'tp')
- new_state: float32 [2, 512, 32, 64], P(None, ('grp', 'ep'), 'tp')
The draws below stay inside these ranges and needn't reach their ends.
Inputs may be any that keep to these rules, and one draw needn't show every extreme that they name: `route_ids`: each row names 6 different experts; within each aligned block of 32 rows no expert is named more than 24 times, and in some block one expert is named exactly 24 times. `norm_gain`: positive gains.
All inputs are finite; a program needn't handle non-finite values.
Results may differ from the reference program's by a relative error of at most 0.015.
Values may be sent and summed in bfloat16 or wider, within the bound.
No kernel may reach another device: no remote copies, remote signals or barrier semaphores. Data moves between devices by JAX's collectives and lax.ppermute only.
A program may use at most 128 MiB of HBM per device.

```python
import math
import jax
import jax.numpy as jnp
import numpy as np
from jax import lax

D = 2048
S5_WIDTH = 512
GROUP = 16
STATE = 64
EFF = 512
DENSE = 1024
TOP_K = 6
SEQ_DEV = 32
GROUPS = 32
EXPERTS = 16
SEQS = 512
CAP = 24
N_EP = 16
N_TP = 2


def draw_norm_gain(key, part):
    ramp = jnp.arange(D, dtype=jnp.float32) / D
    base = jnp.exp(math.log(0.3) + math.log(10.0) * ramp)
    noise = jax.random.uniform(jax.random.fold_in(key, 11), (D,), jnp.float32, 0.7, 1.3)
    return jnp.clip(base * noise, 0.1, 6.0).astype(jnp.float32)


def levels(own_key, dims, cuts, low, top_value):
    level = 1.0
    for axis_at, parts in cuts:
        draws = jax.random.uniform(jax.random.fold_in(jax.random.fold_in(own_key, 6), axis_at), (parts,), jnp.float32, low / len(cuts), top_value / len(cuts))
        level = level * jnp.repeat(jnp.exp(draws), dims[axis_at] // parts).reshape((-1,) + (1,) * (len(dims) - 1 - axis_at))
    return level


def routed_block(rng, own, number, rows, amount, top, reach, skew):
    order = jax.random.permutation(rng, amount)
    crowded, common = portions_of(amount, rows * top, reach, skew, True), portions_of(amount, rows * top, reach, skew, False)
    places = jnp.arange(amount)

    def named(lengths, turn):
        used = int((lengths > 0).sum())
        fixed = max(1, used // 4)
        passed = fixed + (places - fixed + turn * (used - fixed)) % max(1, amount - fixed)
        return jnp.zeros((amount,), jnp.int32).at[order[jnp.where(places < fixed, places, passed)]].set(jnp.asarray(lengths, jnp.int32))

    lengths = jnp.where(number % 4 == 0, named(crowded, number // 4), named(common, number - number // 4 - 1))
    mixed = jax.random.permutation(jax.random.fold_in(own, 3), amount)
    source_of, receiver = mixed[0:amount // 2 * 2:2], mixed[1:amount // 2 * 2:2]
    slack = jnp.minimum(lengths[source_of] - 1, reach - lengths[receiver]) // 2
    slack = jnp.where((source_of == order[0]) | (receiver == order[0]) | (lengths[receiver] == 0), 0, jnp.maximum(slack, 0))
    passed = jax.random.randint(jax.random.fold_in(own, 4), (amount // 2,), 0, 1 << 20) % (slack + 1)
    lengths = lengths.at[source_of].add(-passed).at[receiver].add(passed)
    members = jnp.searchsorted(jnp.cumsum(lengths), jnp.arange(rows * top), side="right").astype(jnp.int32)
    grid = members.reshape(top, rows).T
    grid = grid[jax.random.permutation(jax.random.fold_in(own, 1), rows)]
    turn = jax.random.randint(jax.random.fold_in(own, 2), (rows, 1), 0, top)
    return jnp.take_along_axis(grid, (jnp.arange(top)[None, :] + turn) % top, axis=1)


def portions_of(count, total, limit, skew, full):
    weights = [(1 << 20) // math.isqrt(rank ** skew) + 1 for rank in range(1, count + 1)]
    largest = limit if full else min(limit, max(-(-total // count), total * weights[0] // sum(weights)))
    least = 1 if total - largest >= count - 1 else 0
    counts, surplus = [largest] + [least] * (count - 1), total - largest - least * (count - 1)
    while surplus > 0:
        movable = [i for i in range(1, count) if counts[i] < largest] or [i for i in range(1, count) if counts[i] < limit]
        whole, budget = sum([weights[i] for i in movable]), surplus
        for i in movable:
            addition = min(limit - counts[i], max(1, budget * weights[i] // whole), surplus)
            counts[i] = counts[i] + addition
            surplus = surplus - addition
    return np.array(counts)


def scatter_about(key, dims, scale, most, cuts=(), kind=jnp.bfloat16):
    entries = jax.random.normal(key, dims, jnp.float32) * scale
    if len(cuts) > 0:
        entries = levels(key, dims, cuts, -0.22, 0.18) * entries
    return jnp.clip(entries, min=-most, max=most).astype(kind)


def setup_inputs(seed: int = 0, part: int = 0) -> dict:
    keys = jax.random.split(jax.random.key(seed), 27)
    own_keys = jax.random.split(jax.random.fold_in(keys[26], part), 27)
    layer_input = scatter_about(own_keys[0], (SEQS, D), 1.0, 6.0, ((0, 16),))
    ssm_state = scatter_about(own_keys[1], (2, SEQS, GROUPS, STATE), 0.5, 4.0, ((1, 16), (2, 2)), jnp.float32)
    w_input = scatter_about(keys[2], (D, S5_WIDTH), D ** -0.5, 0.125, ((1, 2),))
    decay_rate = jnp.clip(jnp.exp(math.log(2.0) - 3.6888794 * jax.random.uniform(keys[3], (GROUPS, STATE), jnp.float32) ** levels(keys[3], (GROUPS, STATE), ((0, 2),), -0.2, 0.2)), 0.05, 2.0)
    frequency = jnp.clip(20.0 * jax.random.uniform(keys[4], (GROUPS, STATE), jnp.float32) ** levels(keys[4], (GROUPS, STATE), ((0, 2),), -0.2, 0.2), 0.0, 20.0)
    step_log = jnp.clip(-2.3 + 2.3 * jax.random.uniform(keys[5], (GROUPS,), jnp.float32) ** levels(keys[5], (GROUPS,), ((0, 2),), -0.2, 0.2), -2.3, 0.0)
    input_map = scatter_about(keys[6], (2, GROUPS, STATE, GROUP), (2 * GROUP) ** -0.5, 1.0, ((1, 2),), jnp.float32)
    output_map = scatter_about(keys[7], (2, GROUPS, GROUP, STATE), STATE ** -0.5, 0.75, ((1, 2),), jnp.float32)
    skip_gain = scatter_about(keys[8], (GROUPS, GROUP), 0.5, 3.0, ((0, 2),), jnp.float32)
    glu_weight = scatter_about(keys[9], (S5_WIDTH, S5_WIDTH), S5_WIDTH ** -0.5, 0.25)
    mix_out = scatter_about(keys[10], (S5_WIDTH, D), (S5_WIDTH // 8) ** -0.5, 0.75)
    norm_gain = draw_norm_gain(jax.random.fold_in(keys[26], 71), part)
    norm_shift = scatter_about(keys[12], (D,), 0.3, 2.0, (), jnp.float32)
    route_ids_keys = jax.random.split(jax.random.fold_in(own_keys[13], 1), SEQS // SEQ_DEV)
    route_ids_turns = jax.random.permutation(jax.random.fold_in(own_keys[13], 3), SEQS // SEQ_DEV)
    route_ids = jax.vmap(lambda own, number: routed_block(jax.random.fold_in(own_keys[13], 2), own, number, SEQ_DEV, EXPERTS, TOP_K, CAP, 2))(route_ids_keys, route_ids_turns).reshape((SEQS, TOP_K))
    route_weights = jnp.clip(jnp.exp(math.log(1.0) - 2.3025851 * jax.random.uniform(own_keys[14], (SEQS, TOP_K), jnp.float32) ** levels(own_keys[14], (SEQS, TOP_K), ((0, 16),), -0.2, 0.2)), 0.1, 1.0)
    gate_expert = scatter_about(keys[15], (EXPERTS, D, EFF), D ** -0.5, 0.125, ((0, 16), (2, 2)))
    up_expert = scatter_about(keys[16], (EXPERTS, D, EFF), D ** -0.5, 0.125, ((0, 16), (2, 2)))
    down_expert = scatter_about(keys[17], (EXPERTS, EFF, D), EFF ** -0.5, 0.25, ((0, 16), (1, 2)))
    gate_shared = scatter_about(keys[18], (D, EFF), D ** -0.5, 0.125, ((1, 2),))
    up_shared = scatter_about(keys[19], (D, EFF), D ** -0.5, 0.125, ((1, 2),))
    down_shared = scatter_about(keys[20], (EFF, D), EFF ** -0.5, 0.25, ((0, 2),))
    dense_in = scatter_about(keys[21], (DENSE, D), D ** -0.5, 0.125, ((0, 16),))
    dense_out = scatter_about(keys[22], (DENSE, D), DENSE ** -0.5, 0.1875, ((0, 16), (1, 2)))
    branch_gate = scatter_about(keys[23], (D,), D ** -0.5, 0.125)
    final_gain = jnp.clip(1.0 + 0.18 * jax.random.normal(keys[24], (D,), jnp.float32), 0.1, 1.9)
    final_shift = scatter_about(keys[25], (D,), 0.3, 2.0, ((0, 2),), jnp.float32)
    return dict(layer_input=layer_input, ssm_state=ssm_state, w_input=w_input, decay_rate=decay_rate, frequency=frequency, step_log=step_log, input_map=input_map, output_map=output_map, skip_gain=skip_gain, glu_weight=glu_weight, mix_out=mix_out, norm_gain=norm_gain, norm_shift=norm_shift, route_ids=route_ids, route_weights=route_weights, gate_expert=gate_expert, up_expert=up_expert, down_expert=down_expert, gate_shared=gate_shared, up_shared=up_shared, down_shared=down_shared, dense_in=dense_in, dense_out=dense_out, branch_gate=branch_gate, final_gain=final_gain, final_shift=final_shift)


residual_alpha = 1.681792830507429
route_scale = 2.5
norm_eps = 1e-05
highest = lax.Precision.HIGHEST

def state_update(inputs, ssm_state, decay_rate, frequency, step_log, input_map, output_map, skip_gain):
    step_size = jnp.exp(step_log)[:, None]
    magnitude = jnp.exp(-decay_rate * step_size)
    rotation = frequency * step_size
    decay_re = magnitude * jnp.cos(rotation)
    decay_im = magnitude * jnp.sin(rotation)
    eigen_re = -decay_rate
    denominator = eigen_re * eigen_re + frequency * frequency
    factor_re = ((decay_re - 1.0) * eigen_re + decay_im * frequency) / denominator
    factor_im = (decay_im * eigen_re - (decay_re - 1.0) * frequency) / denominator
    drive_re = factor_re[..., None] * input_map[0] - factor_im[..., None] * input_map[1]
    drive_im = factor_re[..., None] * input_map[1] + factor_im[..., None] * input_map[0]
    pushed_re = jnp.einsum('gpm,tgm->tgp', drive_re, inputs, precision=highest)
    pushed_im = jnp.einsum('gpm,tgm->tgp', drive_im, inputs, precision=highest)
    new_re = decay_re * ssm_state[0] - decay_im * ssm_state[1] + pushed_re
    new_im = decay_re * ssm_state[1] + decay_im * ssm_state[0] + pushed_im
    response = jnp.einsum('gmp,tgp->tgm', output_map[0], new_re, precision=highest) - jnp.einsum('gmp,tgp->tgm', output_map[1], new_im, precision=highest) + skip_gain * inputs
    return (response, jnp.stack([new_re, new_im]))

def layer_norm_rows(values, gain, shift):
    mean = lax.optimization_barrier(jnp.mean(values, axis=1, keepdims=True))
    variance = lax.optimization_barrier(jnp.mean(jnp.square(values - mean), axis=1, keepdims=True))
    return (values - mean) * lax.rsqrt(variance + norm_eps) * gain + shift

def blockwise_down(hidden, down_weight):
    width = hidden.shape[1] // N_TP
    summed = jnp.zeros((hidden.shape[0], down_weight.shape[1]), jnp.float32)
    for portion in range(N_TP):
        part = jnp.dot(hidden[:, portion * width:(portion + 1) * width], down_weight[portion * width:(portion + 1) * width], preferred_element_type=jnp.float32)
        rounded = lax.optimization_barrier(part.astype(jnp.bfloat16))
        summed = summed + rounded.astype(jnp.float32)
    return summed.astype(jnp.bfloat16)

def swiglu_rows(rows, gate_weight, up_weight, down_weight):
    gate_part = jnp.dot(rows, gate_weight, preferred_element_type=jnp.float32)
    up_part = jnp.dot(rows, up_weight, preferred_element_type=jnp.float32)
    hidden = (jax.nn.silu(gate_part) * up_part).astype(jnp.bfloat16)
    return blockwise_down(hidden, down_weight)

def reference(layer_input, ssm_state, w_input, decay_rate, frequency, step_log, input_map, output_map, skip_gain, glu_weight, mix_out, norm_gain, norm_shift, route_ids, route_weights, gate_expert, up_expert, down_expert, gate_shared, up_shared, down_shared, dense_in, dense_out, branch_gate, final_gain, final_shift):
    projected = jnp.dot(layer_input, w_input, preferred_element_type=jnp.float32).astype(jnp.bfloat16)
    inputs = projected.astype(jnp.float32).reshape(SEQS, GROUPS, GROUP)
    response, new_state = state_update(inputs, ssm_state, decay_rate, frequency, step_log, input_map, output_map, skip_gain)
    activated = jax.nn.gelu(response.reshape(SEQS, S5_WIDTH)).astype(jnp.bfloat16)
    glu_out = (activated.astype(jnp.float32) * jax.nn.sigmoid(jnp.dot(activated, glu_weight, preferred_element_type=jnp.float32))).astype(jnp.bfloat16)
    mixed = jnp.dot(glu_out, mix_out, preferred_element_type=jnp.float32).astype(jnp.bfloat16)
    normed = layer_norm_rows(residual_alpha * layer_input.astype(jnp.float32) + mixed.astype(jnp.float32), norm_gain, norm_shift).astype(jnp.bfloat16)
    weights = route_weights / lax.optimization_barrier(jnp.sum(route_weights, axis=1, keepdims=True)) * route_scale
    choices_dev = SEQ_DEV * TOP_K
    block_ids = route_ids.reshape(N_EP, choices_dev)
    hits = (block_ids[..., None] == jnp.arange(EXPERTS, dtype=jnp.int32)).astype(jnp.int32)
    ranks = lax.optimization_barrier(jnp.sum((jnp.cumsum(hits, axis=1) - hits) * hits, axis=2)).astype(jnp.int32)
    sources = jnp.broadcast_to(jnp.arange(N_EP, dtype=jnp.int32)[:, None], (N_EP, choices_dev))
    repeated = jnp.repeat(normed.reshape(N_EP, SEQ_DEV, D), TOP_K, axis=1)
    buffer = jnp.zeros((N_EP, EXPERTS, CAP, D), jnp.bfloat16).at[sources, block_ids, ranks].set(repeated)
    per_expert = jnp.moveaxis(buffer, 1, 0)

    def run_expert(packed):
        slot_rows, gate_weight, up_weight, down_weight = packed
        result = swiglu_rows(slot_rows.reshape(N_EP * CAP, D), gate_weight, up_weight, down_weight)
        return result.reshape(N_EP, CAP, D)
    results = lax.map(run_expert, (per_expert, gate_expert, up_expert, down_expert))
    picked = results[block_ids, sources, ranks].astype(jnp.float32).reshape(SEQS, TOP_K, D)
    routed = lax.optimization_barrier(jnp.sum(picked * weights[:, :, None], axis=1))
    shared = swiglu_rows(normed, gate_shared, up_shared, down_shared)
    dense_hidden = jax.nn.gelu(jnp.dot(normed, dense_in.T, preferred_element_type=jnp.float32)).astype(jnp.bfloat16)
    dense = jnp.dot(dense_hidden, dense_out, preferred_element_type=jnp.float32)
    branch = jax.nn.sigmoid(jnp.dot(normed, branch_gate, preferred_element_type=jnp.float32))
    total = residual_alpha * normed.astype(jnp.float32) + routed + shared.astype(jnp.float32) + branch[:, None] * dense
    mean = lax.optimization_barrier(jnp.mean(total, axis=1, keepdims=True))
    variance = lax.optimization_barrier(jnp.mean(total * total, axis=1, keepdims=True)) - mean * mean
    layer_output = ((total - mean) * lax.rsqrt(variance + norm_eps) * final_gain + final_shift).astype(jnp.bfloat16)
    return (layer_output, new_state)
```

```python
import jax
import jax.numpy as jnp
from jax import lax
from jax.sharding import PartitionSpec as P

residual_alpha = 1.681792830507429
route_scale = 2.5
norm_eps = 1e-05
highest = lax.Precision.HIGHEST
both_axes = ("ep", "tp")


def state_update(
    inputs, ssm_state, decay_rate, frequency, step_log, input_map, output_map, skip_gain
):
    step_size = jnp.exp(step_log)[:, None]
    magnitude = jnp.exp(-decay_rate * step_size)
    rotation = frequency * step_size
    decay_re = magnitude * jnp.cos(rotation)
    decay_im = magnitude * jnp.sin(rotation)
    eigen_re = -decay_rate
    denominator = eigen_re * eigen_re + frequency * frequency
    factor_re = ((decay_re - 1.0) * eigen_re + decay_im * frequency) / denominator
    factor_im = (decay_im * eigen_re - (decay_re - 1.0) * frequency) / denominator
    drive_re = factor_re[..., None] * input_map[0] - factor_im[..., None] * input_map[1]
    drive_im = factor_re[..., None] * input_map[1] + factor_im[..., None] * input_map[0]
    pushed_re = jnp.einsum("gpm,tgm->tgp", drive_re, inputs, precision=highest)
    pushed_im = jnp.einsum("gpm,tgm->tgp", drive_im, inputs, precision=highest)
    new_re = decay_re * ssm_state[0] - decay_im * ssm_state[1] + pushed_re
    new_im = decay_re * ssm_state[1] + decay_im * ssm_state[0] + pushed_im
    response = (
        jnp.einsum("gmp,tgp->tgm", output_map[0], new_re, precision=highest)
        - jnp.einsum("gmp,tgp->tgm", output_map[1], new_im, precision=highest)
        + skip_gain * inputs
    )
    return (response, jnp.stack([new_re, new_im]))


def layer_norm_rows(values, gain, shift):
    mean = jnp.mean(values, axis=1, keepdims=True)
    variance = jnp.mean(jnp.square(values - mean), axis=1, keepdims=True)
    return (values - mean) * lax.rsqrt(variance + norm_eps) * gain + shift

def swap_core(value, count_tp, step=1):
    return lax.ppermute(value, "tp", [(t, (t + step) % count_tp) for t in range(count_tp)])


def split_of(count_ep):
    inner = 1
    while inner < 4 and count_ep % (inner * 2) == 0:
        inner *= 2
    return (count_ep // inner, inner)


def outer_peer(place, step, outer):
    return place ^ step if outer & (outer - 1) == 0 else (place + step) % outer


def line_moves(step, count_ep, count_tp):
    outer, inner = split_of(count_ep)
    moves = []
    for rank in range(count_ep):
        peer = outer_peer(rank // inner, step, outer) * inner + rank % inner
        holder = rank % inner % count_tp
        moves.append((rank * count_tp + holder, peer * count_tp + holder))
    return moves


def plane_moves(step, count_ep, count_tp):
    outer, inner = split_of(count_ep)
    moves = []
    for rank in range(count_ep):
        holder = rank % inner % count_tp
        moves.append((rank * count_tp + holder, (rank ^ step) * count_tp + holder))
    return moves


def backward(moves):
    return [(target, source) for source, target in moves]


def routed_rows(rows, width, own_expert, experts, gates, ups, downs, dense_in, dense_outs, gate_row):
    tokens = rows[:, :width]
    spread = rows[:, width : width + 2 * experts].astype(jnp.float32)
    spread = spread[:, :experts] + spread[:, experts:]
    pieces = []
    halves = []
    for local in range(gates[0].shape[0]):
        share = lax.dynamic_slice_in_dim(spread, own_expert + local, 1, 1)
        for gate, up, down in zip(gates, ups, downs):
            gate_part = jnp.dot(tokens, gate[local], preferred_element_type=jnp.float32)
            up_part = jnp.dot(tokens, up[local], preferred_element_type=jnp.float32)
            pieces.append((jax.nn.silu(gate_part) * up_part * share).astype(jnp.bfloat16))
            halves.append(down[local])
    dense_part = lax.dot_general(
        tokens, dense_in, (((1,), (1,)), ((), ())), preferred_element_type=jnp.float32
    )
    branch = jax.nn.sigmoid(jnp.dot(tokens, gate_row, preferred_element_type=jnp.float32))
    dense_hidden = (jax.nn.gelu(dense_part) * branch[:, None]).astype(jnp.bfloat16)
    total = jnp.dot(dense_hidden, dense_outs, preferred_element_type=jnp.float32)
    for piece, half in zip(pieces, halves):
        total = total + jnp.dot(piece, half, preferred_element_type=jnp.float32)
    return total.astype(jnp.bfloat16)


def in_core_order(pieces, core):
    ordered = jnp.concatenate([pieces[-place % len(pieces)] for place in range(len(pieces))], axis=1)
    for turn in range(1, len(pieces)):
        turned = [pieces[(turn - place) % len(pieces)] for place in range(len(pieces))]
        ordered = jnp.where(core == turn, jnp.concatenate(turned, axis=1), ordered)
    return ordered


def body(
    layer_input,
    ssm_state,
    w_input,
    decay_rate,
    frequency,
    step_log,
    input_map,
    output_map,
    skip_gain,
    glu_weight,
    mix_out,
    norm_gain,
    norm_shift,
    route_ids,
    route_weights,
    gate_expert,
    up_expert,
    down_expert,
    gate_shared,
    up_shared,
    down_shared,
    dense_in,
    dense_out,
    branch_gate,
    final_gain,
    final_shift,
):
    count_ep = lax.axis_size("ep")
    count_tp = lax.axis_size("tp")
    core = lax.axis_index("tp")
    rank = lax.axis_index("ep")
    outer, inner = split_of(count_ep)
    holder = lax.rem(lax.rem(rank, inner), count_tp)
    is_holder = core == holder
    gates, ups, downs = [gate_expert], [up_expert], [down_expert]
    out_pieces, norm_pieces = [dense_out], [jnp.stack([final_gain, final_shift])]
    for step in range(1, count_tp):
        for kept in (gates, ups, downs, out_pieces, norm_pieces):
            kept.append(swap_core(kept[0], count_tp, step))
    dense_outs = in_core_order(out_pieces, core)
    final_pair = in_core_order(norm_pieces, core)
    seq_rows, width = layer_input.shape
    local_groups, channels = skip_gain.shape
    projected = jnp.dot(layer_input, w_input, preferred_element_type=jnp.float32).astype(
        jnp.bfloat16
    )
    inputs = projected.astype(jnp.float32).reshape(seq_rows, local_groups, channels)
    response, new_state = state_update(
        inputs, ssm_state, decay_rate, frequency, step_log, input_map, output_map, skip_gain
    )
    activated = jax.nn.gelu(response.reshape(seq_rows, local_groups * channels)).astype(
        jnp.bfloat16
    )
    every_channel = lax.all_gather(activated, "tp", axis=1, tiled=True)
    glu_out = (
        every_channel.astype(jnp.float32)
        * jax.nn.sigmoid(jnp.dot(every_channel, glu_weight, preferred_element_type=jnp.float32))
    ).astype(jnp.bfloat16)
    mixed = jnp.dot(glu_out, mix_out, preferred_element_type=jnp.float32).astype(jnp.bfloat16)
    normed = layer_norm_rows(
        residual_alpha * layer_input.astype(jnp.float32) + mixed.astype(jnp.float32),
        norm_gain,
        norm_shift,
    ).astype(jnp.bfloat16)
    top_k = route_ids.shape[1]
    local_experts = gate_expert.shape[0]
    experts = local_experts * count_ep
    weights = route_weights / jnp.sum(route_weights, axis=1, keepdims=True) * route_scale
    named = route_ids[:, :, None] == jnp.arange(experts, dtype=jnp.int32)[None, None, :]
    spread = jnp.sum(jnp.where(named, weights[:, :, None], 0.0), axis=1)
    spread_high = spread.astype(jnp.bfloat16)
    spread_low = (spread - spread_high.astype(jnp.float32)).astype(jnp.bfloat16)
    padding = jnp.zeros((seq_rows, -2 * experts % 128), jnp.bfloat16)
    packet = jnp.concatenate([normed, spread_high, spread_low, padding], axis=1)
    line = [packet]
    for step in range(1, outer):
        line.append(lax.ppermute(packet, both_axes, line_moves(step, count_ep, count_tp)))
    line = jnp.concatenate(line, axis=0)
    arrived = [line]
    for step in range(1, inner):
        arrived.append(lax.ppermute(line, both_axes, plane_moves(step, count_ep, count_tp)))
    shared_gate = jnp.dot(normed, gate_shared, preferred_element_type=jnp.float32)
    shared_up = jnp.dot(normed, up_shared, preferred_element_type=jnp.float32)
    shared_hidden = (jax.nn.silu(shared_gate) * shared_up).astype(jnp.bfloat16)
    shared = jnp.dot(shared_hidden, down_shared, preferred_element_type=jnp.float32)
    shared_sent = shared.astype(jnp.bfloat16)
    for step in range(1, count_tp):
        shared = shared + swap_core(shared_sent, count_tp, step).astype(jnp.float32)
    offset = lax.rem(core - holder + count_tp, count_tp)
    results = []
    for slot in range(inner // count_tp):
        rows = arrived[slot * count_tp]
        for step in range(1, count_tp):
            rows = jnp.where(offset == step, arrived[slot * count_tp + step], rows)
        results.append(
            routed_rows(
                rows,
                width,
                rank * local_experts,
                experts,
                gates,
                ups,
                downs,
                dense_in,
                dense_outs,
                branch_gate,
            )
        )
    gathered = results[0].astype(jnp.float32)
    for step in range(1, inner):
        moves = backward(plane_moves(step, count_ep, count_tp))
        gathered = gathered + lax.ppermute(results[step // count_tp], both_axes, moves).astype(
            jnp.float32
        )
    blocks = gathered.reshape(outer, seq_rows, width)
    sent_blocks = blocks.astype(jnp.bfloat16)
    summed = blocks[0]
    for step in range(1, outer):
        moves = backward(line_moves(step, count_ep, count_tp))
        summed = summed + lax.ppermute(sent_blocks[step], both_axes, moves).astype(jnp.float32)
    total = residual_alpha * normed.astype(jnp.float32) + summed + shared
    mean = jnp.mean(total, axis=1, keepdims=True)
    variance = jnp.mean(total * total, axis=1, keepdims=True) - mean * mean
    finished = (
        (total - mean) * lax.rsqrt(variance + norm_eps) * final_pair[:1] + final_pair[1:]
    ).astype(jnp.bfloat16)
    half_width = width // count_tp
    layer_output = lax.dynamic_slice_in_dim(finished, core * half_width, half_width, 1)
    for step in range(1, count_tp):
        moves = [
            (
                r * count_tp + r % inner % count_tp,
                r * count_tp + (r % inner % count_tp + step) % count_tp,
            )
            for r in range(count_ep)
        ]
        far = lax.rem(core + step, count_tp) * half_width
        far_half = lax.dynamic_slice_in_dim(finished, far, half_width, 1)
        layer_output = jnp.where(
            offset == step, lax.ppermute(far_half, both_axes, moves), layer_output
        )
    return (layer_output, new_state)


def solution(mesh):
    placed = (
        P(("grp", "ep"), None),
        P(None, ("grp", "ep"), "tp", None),
        P(None, "tp"),
        P("tp", None),
        P("tp", None),
        P("tp"),
        P(None, "tp", None, None),
        P(None, "tp", None, None),
        P("tp", None),
        P(),
        P(),
        P(),
        P(),
        P(("grp", "ep"), None),
        P(("grp", "ep"), None),
        P("ep", None, "tp"),
        P("ep", None, "tp"),
        P("ep", "tp", None),
        P(None, "tp"),
        P(None, "tp"),
        P("tp", None),
        P("ep", None),
        P("ep", "tp"),
        P(),
        P("tp"),
        P("tp"),
    )
    return jax.shard_map(
        body,
        mesh=mesh,
        in_specs=placed,
        out_specs=(P(("grp", "ep"), "tp"), P(None, ("grp", "ep"), "tp", None)),
        check_vma=False,
    )
```

```python
import functools

import jax
import jax.numpy as jnp
from jax import lax
from jax.experimental import pallas as pl
from jax.experimental.pallas import tpu as pltpu
from jax.sharding import PartitionSpec as P


residual_alpha = 1.681792830507429
route_scale = 2.5
norm_eps = 1e-05
highest = lax.Precision.HIGHEST
both_axes = ("ep", "tp")


def state_update(
    inputs, ssm_state, decay_rate, frequency, step_log, input_map, output_map, skip_gain
):
    step_size = jnp.exp(step_log)[:, None]
    magnitude = jnp.exp(-decay_rate * step_size)
    rotation = frequency * step_size
    decay_re = magnitude * jnp.cos(rotation)
    decay_im = magnitude * jnp.sin(rotation)
    eigen_re = -decay_rate
    denominator = eigen_re * eigen_re + frequency * frequency
    factor_re = ((decay_re - 1.0) * eigen_re + decay_im * frequency) / denominator
    factor_im = (decay_im * eigen_re - (decay_re - 1.0) * frequency) / denominator
    drive_re = factor_re[..., None] * input_map[0] - factor_im[..., None] * input_map[1]
    drive_im = factor_re[..., None] * input_map[1] + factor_im[..., None] * input_map[0]
    pushed_re = jnp.einsum("gpm,tgm->tgp", drive_re, inputs, precision=highest)
    pushed_im = jnp.einsum("gpm,tgm->tgp", drive_im, inputs, precision=highest)
    new_re = decay_re * ssm_state[0] - decay_im * ssm_state[1] + pushed_re
    new_im = decay_re * ssm_state[1] + decay_im * ssm_state[0] + pushed_im
    response = (
        jnp.einsum("gmp,tgp->tgm", output_map[0], new_re, precision=highest)
        - jnp.einsum("gmp,tgp->tgm", output_map[1], new_im, precision=highest)
        + skip_gain * inputs
    )
    return (response, jnp.stack([new_re, new_im]))


def split_of(count_ep):
    inner = 1
    while inner < 4 and count_ep % (inner * 2) == 0:
        inner *= 2
    return (count_ep // inner, inner)


def outer_peer(place, step, outer):
    return place ^ step if outer & (outer - 1) == 0 else (place + step) % outer


def line_moves(step, count_ep, count_tp):
    outer, inner = split_of(count_ep)
    moves = []
    for rank in range(count_ep):
        peer = outer_peer(rank // inner, step, outer) * inner + rank % inner
        moves += [(rank * count_tp + t, peer * count_tp + t) for t in range(count_tp)]
    return moves


def plane_moves(step, count_ep, count_tp):
    moves = []
    for rank in range(count_ep):
        moves += [(rank * count_tp + t, (rank ^ step) * count_tp + t) for t in range(count_tp)]
    return moves


def backward(moves):
    return [(target, source) for source, target in moves]


vmem = pl.BlockSpec(memory_space=pltpu.VMEM)
smem = pl.BlockSpec(memory_space=pltpu.SMEM)
anywhere = pl.BlockSpec(memory_space=pl.ANY)


def product(left, right):
    return jnp.dot(left, right, preferred_element_type=jnp.float32)


def params(mebibytes):
    return pltpu.CompilerParams(vmem_limit_bytes=mebibytes << 20)


def cost(flops, moved):
    return pl.CostEstimate(flops=flops, bytes_accessed=moved, transcendentals=0)


def token_half(ref, flipped):
    half = ref.shape[0] // 2
    return jnp.where(flipped, ref[half:, :], ref[:half, :])


def mix_kernel(
    experts,
    core_ref,
    own_ref,
    far_ref,
    glu_ref,
    mix_ref,
    input_ref,
    gain_ref,
    shift_ref,
    ids_ref,
    scores_ref,
    packet_ref,
):
    width = input_ref.shape[1]
    flipped = core_ref[0] == 1
    own, far = token_half(own_ref, flipped), far_ref[...]
    every = jnp.concatenate([jnp.where(flipped, far, own), jnp.where(flipped, own, far)], axis=1)
    gated = (every.astype(jnp.float32) * jax.nn.sigmoid(product(every, glu_ref[...]))).astype(
        jnp.bfloat16
    )
    mixed = product(gated, mix_ref[...]).astype(jnp.bfloat16).astype(jnp.float32)
    values = residual_alpha * token_half(input_ref, flipped).astype(jnp.float32) + mixed
    mean = jnp.mean(values, axis=1, keepdims=True)
    centered = values - mean
    variance = jnp.mean(centered * centered, axis=1, keepdims=True)
    normed = centered * lax.rsqrt(variance + norm_eps) * gain_ref[...] + shift_ref[...]
    packet_ref[:, :width] = normed.astype(jnp.bfloat16)
    scores = token_half(scores_ref, flipped)
    ids = token_half(ids_ref, flipped)
    weights = scores / jnp.sum(scores, axis=1, keepdims=True) * route_scale
    rows, extra = packet_ref.shape[0], packet_ref.shape[1] - width
    lane = lax.broadcasted_iota(jnp.int32, (rows, extra), 1)
    expert = jnp.where(lane < experts, lane, lane - experts)
    spread = jnp.zeros((rows, extra), jnp.float32)
    for choice in range(scores.shape[1]):
        named = ids[:, choice : choice + 1] == expert
        spread = spread + jnp.where(named, weights[:, choice : choice + 1], 0.0)
    high = spread.astype(jnp.bfloat16).astype(jnp.float32)
    packet_ref[:, width:] = jnp.where(lane < experts, high, spread - high).astype(jnp.bfloat16)


def shared_kernel(own_ref, far_ref, gate_hbm, up_hbm, down_hbm, own_out, far_out, *scratch):
    gate_ref, up_ref, down_ref, sems = scratch
    copies = []
    for index, (source, target) in enumerate(zip((gate_hbm, up_hbm, down_hbm), scratch)):
        copies.append(pltpu.make_async_copy(source, target, sems.at[index]))
        copies[-1].start()
    width, half = own_out.shape[1], own_out.shape[0]
    normed = jnp.concatenate([own_ref[:, :width], far_ref[:, :width]], axis=0)
    copies[0].wait()
    gate_part = product(normed, gate_ref[...])
    copies[1].wait()
    hidden = (jax.nn.silu(gate_part) * product(normed, up_ref[...])).astype(jnp.bfloat16)
    copies[2].wait()
    result = product(hidden, down_ref[...]).astype(jnp.bfloat16)
    own_out[...] = result[:half]
    far_out[...] = result[half:]


def join_kernel(*refs):
    rows = refs[0].shape[0]
    for place, ref in enumerate(refs[:-1]):
        refs[-1][place * rows : (place + 1) * rows, :] = ref[...]


def sum_kernel(count, *refs):
    rows = refs[count].shape[0]
    for place, out_ref in enumerate(refs[count:]):
        total = refs[0][place * rows : (place + 1) * rows, :].astype(jnp.float32)
        for ref in refs[1:count]:
            total = total + ref[place * rows : (place + 1) * rows, :].astype(jnp.float32)
        out_ref[...] = total.astype(jnp.bfloat16)


def final_kernel(count, core_ref, packet_ref, own_norm_ref, far_norm_ref, *refs):
    own_ref, far_ref = refs[count:]
    half = own_ref.shape[1]
    flipped = core_ref[0] == 1
    total = residual_alpha * packet_ref[:, : 2 * half].astype(jnp.float32)
    for ref in refs[:count]:
        total = total + ref[...].astype(jnp.float32)
    mean = jnp.mean(total, axis=1, keepdims=True)
    variance = jnp.mean(total * total, axis=1, keepdims=True) - mean * mean
    scaled = (total - mean) * lax.rsqrt(variance + norm_eps)
    left, right = scaled[:, :half], scaled[:, half:]
    own = jnp.where(flipped, right, left)
    far = jnp.where(flipped, left, right)
    own_ref[...] = (own * own_norm_ref[:1] + own_norm_ref[1:]).astype(jnp.bfloat16)
    far_ref[...] = (far * far_norm_ref[:1] + far_norm_ref[1:]).astype(jnp.bfloat16)


def place_kernel(core_ref, own_ref, far_ref, out_ref):
    rows = own_ref.shape[0]
    flipped = core_ref[0] == 1
    own, far = own_ref[...], far_ref[...]
    out_ref[:rows, :] = jnp.where(flipped, far, own)
    out_ref[rows:, :] = jnp.where(flipped, own, far)


def routed_kernel(width, experts, local, place_ref, first_ref, second_ref, branch_ref, *refs):
    weights, outs = refs[:9], refs[9:11]
    held, sems = refs[11:20], refs[20]
    copies = [
        pltpu.make_async_copy(source, target, sems.at[index])
        for index, (source, target) in enumerate(zip(weights, held))
    ]
    for copy in copies:
        copy.start()
    own_expert, core = place_ref[0], place_ref[1]
    rows = jnp.concatenate([first_ref[...], second_ref[...]], axis=0)
    block = first_ref.shape[0]
    tokens = rows[:, :width]
    spread = rows[:, width:].astype(jnp.float32)
    lane = lax.broadcasted_iota(jnp.int32, spread.shape, 1)
    shares = []
    for index in range(local):
        chosen = (lane == own_expert + index) | (lane == own_expert + index + experts)
        shares.append(jnp.sum(jnp.where(chosen, spread, 0.0), axis=1, keepdims=True))
    logit = jnp.sum(
        tokens.astype(jnp.float32) * branch_ref[...].astype(jnp.float32), axis=1, keepdims=True
    )
    hidden = []
    for side in range(2):
        copies[2 * side].wait()
        copies[2 * side + 1].wait()
        for index in range(local):
            gate_part = product(tokens, held[2 * side][index])
            up_part = product(tokens, held[2 * side + 1][index])
            piece = jax.nn.silu(gate_part) * up_part * shares[index]
            hidden.append((piece.astype(jnp.bfloat16), held[4 + side], index))
    copies[6].wait()
    dense_part = lax.dot_general(
        tokens, held[6][...], (((1,), (1,)), ((), ())), preferred_element_type=jnp.float32
    )
    dense_hidden = (jax.nn.gelu(dense_part) * jax.nn.sigmoid(logit)).astype(jnp.bfloat16)
    for index in (4, 5, 7, 8):
        copies[index].wait()
    part = width // 2
    for side in range(2):
        own_side = core == side
        columns = jnp.where(own_side, held[7][...], held[8][...])
        for start in range(0, part, min(part, 512)):
            stop = min(start + 512, part)
            total = product(dense_hidden, columns[:, start:stop])
            low, high = side * part + start, side * part + stop
            for piece, down, index in hidden:
                total = total + product(piece, down[index, :, low:high])
            rounded = total.astype(jnp.bfloat16)
            outs[0][:, low:high] = rounded[:block]
            outs[1][:, low:high] = rounded[block:]


def routed_rows(width, place, first, second, branch_gate, experts, weights):
    rows = first.shape[0]
    return pl.pallas_call(
        functools.partial(routed_kernel, width, experts, weights[0].shape[0]),
        out_shape=[jax.ShapeDtypeStruct((rows, width), jnp.bfloat16)] * 2,
        in_specs=[smem, vmem, vmem, vmem] + [anywhere] * len(weights),
        out_specs=[vmem] * 2,
        scratch_shapes=[pltpu.VMEM(value.shape, value.dtype) for value in weights]
        + [pltpu.SemaphoreType.DMA((len(weights),))],
        compiler_params=params(28),
        cost_estimate=cost(24 * rows * weights[0].size, 8 << 20),
        name="routed_rows",
    )(place, first, second, branch_gate[None, :], *weights)


def body(
    layer_input,
    ssm_state,
    w_input,
    decay_rate,
    frequency,
    step_log,
    input_map,
    output_map,
    skip_gain,
    glu_weight,
    mix_out,
    norm_gain,
    norm_shift,
    route_ids,
    route_weights,
    gate_expert,
    up_expert,
    down_expert,
    gate_shared,
    up_shared,
    down_shared,
    dense_in,
    dense_out,
    branch_gate,
    final_gain,
    final_shift,
):
    count_ep = lax.axis_size("ep")
    count_tp = lax.axis_size("tp")
    core = lax.axis_index("tp")
    rank = lax.axis_index("ep")
    outer, inner = split_of(count_ep)
    seq_rows, width = layer_input.shape
    local_groups, channels = skip_gain.shape
    local_experts = gate_expert.shape[0]
    experts = local_experts * count_ep
    place = jnp.stack([rank * local_experts, core]).astype(jnp.int32)
    core_word = core.astype(jnp.int32)[None]

    def swapped(value):
        return lax.ppermute(value, "tp", [(t, 1 - t) for t in range(count_tp)])

    def moved(value, moves):
        return lax.ppermute(value, both_axes, moves)

    norm_own = jnp.stack([final_gain, final_shift])
    gate_far = swapped(gate_expert)
    up_far = swapped(up_expert)
    down_far = swapped(down_expert)
    dense_far = swapped(dense_out)
    norm_far = swapped(norm_own)
    projected = jnp.dot(layer_input, w_input, preferred_element_type=jnp.float32).astype(
        jnp.bfloat16
    )
    inputs = projected.astype(jnp.float32).reshape(seq_rows, local_groups, channels)
    response, new_state = state_update(
        inputs, ssm_state, decay_rate, frequency, step_log, input_map, output_map, skip_gain
    )
    activated = jax.nn.gelu(response.reshape(seq_rows, local_groups * channels)).astype(
        jnp.bfloat16
    )
    core_rows = seq_rows // count_tp
    far_tokens = lax.dynamic_slice_in_dim(activated, (1 - core) * core_rows, core_rows, 0)
    activated_far = swapped(far_tokens)
    packet_width = width + -(-2 * experts // 128) * 128
    packet_shape = jax.ShapeDtypeStruct((core_rows, packet_width), jnp.bfloat16)
    row_shape = jax.ShapeDtypeStruct((core_rows, width), jnp.bfloat16)
    packet = pl.pallas_call(
        functools.partial(mix_kernel, experts),
        out_shape=packet_shape,
        in_specs=[smem] + [vmem] * 9,
        out_specs=vmem,
        compiler_params=params(12),
        cost_estimate=cost(2 * seq_rows * (glu_weight.size + mix_out.size), 3 << 20),
        name="mix",
    )(
        core_word,
        activated,
        activated_far,
        glu_weight,
        mix_out,
        layer_input,
        norm_gain[None, :],
        norm_shift[None, :],
        route_ids,
        route_weights,
    )
    packet_far = swapped(packet)
    line = [packet]
    for step in range(1, outer):
        line.append(moved(packet, line_moves(step, count_ep, count_tp)))
    line = pl.pallas_call(
        join_kernel,
        out_shape=jax.ShapeDtypeStruct((outer * core_rows, packet_width), jnp.bfloat16),
        in_specs=[vmem] * outer,
        out_specs=vmem,
        compiler_params=params(12),
        cost_estimate=cost(outer * core_rows * packet_width, 1 << 20),
        name="join",
    )(*line)
    arrived = [line]
    for step in range(1, inner):
        arrived.append(moved(line, plane_moves(step, count_ep, count_tp)))
    held = (gate_shared, up_shared, down_shared)
    shared, shared_sent = pl.pallas_call(
        shared_kernel,
        out_shape=[row_shape] * 2,
        in_specs=[vmem] * 2 + [anywhere] * 3,
        out_specs=[vmem] * 2,
        scratch_shapes=[pltpu.VMEM(value.shape, value.dtype) for value in held]
        + [pltpu.SemaphoreType.DMA((3,))],
        compiler_params=params(12),
        cost_estimate=cost(6 * seq_rows * gate_shared.size, 3 << 20),
        name="shared_mlp",
    )(packet, packet_far, *held)
    shared_far = swapped(shared_sent)
    weights = [gate_expert, up_expert, gate_far, up_far, down_expert, down_far]
    weights += [dense_in, dense_out, dense_far]
    results = []
    for slot in range(inner // 2):
        first, second = arrived[slot * 2 : slot * 2 + 2]
        results += routed_rows(width, place, first, second, branch_gate, experts, weights)
    parts = [results[0]]
    for step in range(1, inner):
        moves = backward(plane_moves(step, count_ep, count_tp))
        parts.append(moved(results[step], moves))
    blocks = pl.pallas_call(
        functools.partial(sum_kernel, inner),
        out_shape=[row_shape] * outer,
        in_specs=[vmem] * inner,
        out_specs=[vmem] * outer,
        compiler_params=params(12),
        cost_estimate=cost(inner * outer * core_rows * width, 3 << 20),
        name="total",
    )(*parts)
    terms = [blocks[0]]
    for step in range(1, outer):
        moves = backward(line_moves(step, count_ep, count_tp))
        terms.append(moved(blocks[step], moves))
    half_shape = jax.ShapeDtypeStruct((core_rows, width // count_tp), jnp.bfloat16)
    terms += [shared, shared_far]
    own_half, far_half = pl.pallas_call(
        functools.partial(final_kernel, len(terms)),
        out_shape=[half_shape] * 2,
        in_specs=[smem] + [vmem] * (3 + len(terms)),
        out_specs=[vmem] * 2,
        compiler_params=params(12),
        cost_estimate=cost(10 * core_rows * width, 1 << 20),
        name="final",
    )(core_word, packet, norm_own, norm_far, *terms)
    handed = swapped(far_half)
    layer_output = pl.pallas_call(
        place_kernel,
        out_shape=jax.ShapeDtypeStruct((seq_rows, width // count_tp), jnp.bfloat16),
        in_specs=[smem, vmem, vmem],
        out_specs=vmem,
        compiler_params=params(12),
        cost_estimate=cost(seq_rows * width, 1 << 18),
        name="place",
    )(core_word, own_half, handed)
    return (layer_output, new_state)


def solution(mesh):
    placed = (
        P(("grp", "ep"), None),
        P(None, ("grp", "ep"), "tp", None),
        P(None, "tp"),
        P("tp", None),
        P("tp", None),
        P("tp"),
        P(None, "tp", None, None),
        P(None, "tp", None, None),
        P("tp", None),
        P(),
        P(),
        P(),
        P(),
        P(("grp", "ep"), None),
        P(("grp", "ep"), None),
        P("ep", None, "tp"),
        P("ep", None, "tp"),
        P("ep", "tp", None),
        P(None, "tp"),
        P(None, "tp"),
        P("tp", None),
        P("ep", None),
        P("ep", "tp"),
        P(),
        P("tp"),
        P("tp"),
    )
    return jax.shard_map(
        body,
        mesh=mesh,
        in_specs=placed,
        out_specs=(P(("grp", "ep"), "tp"), P(None, ("grp", "ep"), "tp", None)),
        check_vma=False,
    )
```

```python
import functools

import jax
import jax.numpy as jnp
from jax import lax
from jax.experimental import pallas as pl
from jax.experimental.pallas import tpu as pltpu
from jax.sharding import PartitionSpec as P


residual_alpha = 1.681792830507429
route_scale = 2.5
norm_eps = 1e-05
both_axes = ("ep", "tp")


def split_of(count_ep):
    inner = 1
    while inner < 4 and count_ep % (inner * 2) == 0:
        inner *= 2
    return (count_ep // inner, inner)


def outer_peer(place, step, outer):
    return place ^ step if outer & (outer - 1) == 0 else (place + step) % outer


def line_moves(step, count_ep, count_tp):
    outer, inner = split_of(count_ep)
    moves = []
    for rank in range(count_ep):
        peer = outer_peer(rank // inner, step, outer) * inner + rank % inner
        moves += [(rank * count_tp + t, peer * count_tp + t) for t in range(count_tp)]
    return moves


def plane_moves(step, count_ep, count_tp):
    moves = []
    for rank in range(count_ep):
        moves += [(rank * count_tp + t, (rank ^ step) * count_tp + t) for t in range(count_tp)]
    return moves


def backward(moves):
    return [(target, source) for source, target in moves]


vmem = pl.BlockSpec(memory_space=pltpu.VMEM)
smem = pl.BlockSpec(memory_space=pltpu.SMEM)
in_hbm = pl.BlockSpec(memory_space=pltpu.HBM)


def product(left, right):
    return jnp.dot(left, right, preferred_element_type=jnp.float32)


def params(mebibytes):
    return pltpu.CompilerParams(vmem_limit_bytes=mebibytes << 20)


def cost(flops, moved):
    return pl.CostEstimate(flops=flops, bytes_accessed=moved, transcendentals=0)


def token_half(ref, flipped):
    half = ref.shape[0] // 2
    return jnp.where(flipped, ref[half:, :], ref[:half, :])


def halves(value):
    high = value.astype(jnp.bfloat16)
    return high, (value - high.astype(jnp.float32)).astype(jnp.bfloat16)


def mixer_kernel(core_ref, *refs):
    sources, (own_ref, far_ref, new_ref) = refs[:9], refs[9:12]
    held, sems = refs[12:21], refs[21]
    copies = []
    for index, (source, target) in enumerate(zip(sources, held)):
        copies.append(pltpu.make_async_copy(source, target, sems.at[index]))
        copies[-1].start()
    step_ref, rate_ref, frequency_ref, input_ref, project_ref, drive_ref, state_ref, readout_ref, skip_ref = held
    rows = input_ref.shape[0]
    groups, _ = rate_ref.shape
    channels = skip_ref.shape[1]
    for copy in copies[:3]:
        copy.wait()
    square = lax.broadcasted_iota(jnp.int32, (groups, groups), 0) == lax.broadcasted_iota(
        jnp.int32, (groups, groups), 1
    )
    step_size = jnp.exp(jnp.sum(jnp.where(square, step_ref[...], 0.0), axis=1, keepdims=True))
    rate, frequency = rate_ref[...], frequency_ref[...]
    magnitude = jnp.exp(-rate * step_size)
    rotation = frequency * step_size
    decay_re = magnitude * jnp.cos(rotation)
    decay_im = magnitude * jnp.sin(rotation)
    denominator = rate * rate + frequency * frequency
    factor_re = (decay_im * frequency - (decay_re - 1.0) * rate) / denominator
    factor_im = (-decay_im * rate - (decay_re - 1.0) * frequency) / denominator
    for copy in copies[3:]:
        copy.wait()
    flipped = core_ref[0] == 1
    projected = product(input_ref[...], project_ref[...]).astype(jnp.bfloat16)
    responses = []
    for index in range(groups):
        one = slice(index, index + 1)
        inputs = projected[:, index * channels : (index + 1) * channels]
        twice = jnp.concatenate([inputs, inputs], axis=1)
        map_re, map_im = drive_ref[0, index], drive_ref[1, index]
        drive_re = halves(factor_re[one] * map_re - factor_im[one] * map_im)
        drive_im = halves(factor_re[one] * map_im + factor_im[one] * map_re)
        old_re = state_ref[pl.ds(index, rows, groups), :]
        old_im = state_ref[pl.ds(rows * groups + index, rows, groups), :]
        new_re = decay_re[one] * old_re - decay_im[one] * old_im
        new_im = decay_re[one] * old_im + decay_im[one] * old_re
        new_re = new_re + product(twice, jnp.concatenate(drive_re, axis=0))
        new_im = new_im + product(twice, jnp.concatenate(drive_im, axis=0))
        new_ref[pl.ds(index, rows, groups), :] = new_re
        new_ref[pl.ds(rows * groups + index, rows, groups), :] = new_im
        high, low = halves(jnp.concatenate([new_re, new_im], axis=1))
        readout = jnp.concatenate([readout_ref[0, index], -readout_ref[1, index]], axis=1)
        read_high, read_low = halves(readout)
        response = lax.dot_general(
            jnp.concatenate([high, low, high], axis=1),
            jnp.concatenate([read_high, read_high, read_low], axis=1),
            (((1,), (1,)), ((), ())),
            preferred_element_type=jnp.float32,
        )
        responses.append(response + skip_ref[one, :] * inputs.astype(jnp.float32))
    activated = jax.nn.gelu(jnp.concatenate(responses, axis=1)).astype(jnp.bfloat16)
    own_ref[...] = jnp.where(flipped, activated[rows // 2 :], activated[: rows // 2])
    far_ref[...] = jnp.where(flipped, activated[: rows // 2], activated[rows // 2 :])


def load_kernel(count, *refs):
    sems = refs[2 * count]
    copies = []
    for index in range(count):
        copies.append(pltpu.make_async_copy(refs[index], refs[count + index], sems.at[index]))
        copies[-1].start()
    for copy in copies:
        copy.wait()


def loaded(values):
    return pl.pallas_call(
        functools.partial(load_kernel, len(values)),
        out_shape=[jax.ShapeDtypeStruct(value.shape, value.dtype) for value in values],
        in_specs=[in_hbm] * len(values),
        out_specs=[vmem] * len(values),
        scratch_shapes=[pltpu.SemaphoreType.DMA((len(values),))],
        compiler_params=params(12),
        cost_estimate=cost(1 << 22, 8 << 20),
        name="load",
    )(*values)


def mix_kernel(
    experts,
    core_ref,
    own_ref,
    far_ref,
    glu_ref,
    mix_ref,
    input_ref,
    gain_ref,
    shift_ref,
    ids_ref,
    scores_ref,
    packet_ref,
):
    width = input_ref.shape[1]
    flipped = core_ref[0] == 1
    own, far = own_ref[...], far_ref[...]
    every = jnp.concatenate([jnp.where(flipped, far, own), jnp.where(flipped, own, far)], axis=1)
    gated = (every.astype(jnp.float32) * jax.nn.sigmoid(product(every, glu_ref[...]))).astype(
        jnp.bfloat16
    )
    mixed = product(gated, mix_ref[...]).astype(jnp.bfloat16).astype(jnp.float32)
    values = residual_alpha * token_half(input_ref, flipped).astype(jnp.float32) + mixed
    mean = jnp.mean(values, axis=1, keepdims=True)
    centered = values - mean
    variance = jnp.mean(centered * centered, axis=1, keepdims=True)
    normed = centered * lax.rsqrt(variance + norm_eps) * gain_ref[...] + shift_ref[...]
    packet_ref[:, :width] = normed.astype(jnp.bfloat16)
    scores = token_half(scores_ref, flipped)
    ids = token_half(ids_ref, flipped)
    weights = scores / jnp.sum(scores, axis=1, keepdims=True) * route_scale
    rows, extra = packet_ref.shape[0], packet_ref.shape[1] - width
    lane = lax.broadcasted_iota(jnp.int32, (rows, extra), 1)
    expert = jnp.where(lane < experts, lane, lane - experts)
    spread = jnp.zeros((rows, extra), jnp.float32)
    for choice in range(scores.shape[1]):
        named = ids[:, choice : choice + 1] == expert
        spread = spread + jnp.where(named, weights[:, choice : choice + 1], 0.0)
    high = spread.astype(jnp.bfloat16).astype(jnp.float32)
    packet_ref[:, width:] = jnp.where(lane < experts, high, spread - high).astype(jnp.bfloat16)


def shared_kernel(own_ref, far_ref, gate_hbm, up_hbm, down_hbm, own_out, far_out, *scratch):
    gate_ref, up_ref, down_ref, sems = scratch
    copies = []
    for index, (source, target) in enumerate(zip((gate_hbm, up_hbm, down_hbm), scratch)):
        copies.append(pltpu.make_async_copy(source, target, sems.at[index]))
        copies[-1].start()
    width, half = own_out.shape[1], own_out.shape[0]
    normed = jnp.concatenate([own_ref[:, :width], far_ref[:, :width]], axis=0)
    copies[0].wait()
    gate_part = product(normed, gate_ref[...])
    copies[1].wait()
    hidden = (jax.nn.silu(gate_part) * product(normed, up_ref[...])).astype(jnp.bfloat16)
    copies[2].wait()
    result = product(hidden, down_ref[...]).astype(jnp.bfloat16)
    own_out[...] = result[:half]
    far_out[...] = result[half:]


def join_kernel(*refs):
    rows = refs[0].shape[0]
    for place, ref in enumerate(refs[:-1]):
        refs[-1][place * rows : (place + 1) * rows, :] = ref[...]


def sum_kernel(count, *refs):
    rows = refs[count].shape[0]
    for place, out_ref in enumerate(refs[count:]):
        total = refs[0][place * rows : (place + 1) * rows, :].astype(jnp.float32)
        for ref in refs[1:count]:
            total = total + ref[place * rows : (place + 1) * rows, :].astype(jnp.float32)
        out_ref[...] = total.astype(jnp.bfloat16)


def final_kernel(count, core_ref, packet_ref, own_norm_ref, far_norm_ref, *refs):
    own_ref, far_ref = refs[count:]
    half = own_ref.shape[1]
    flipped = core_ref[0] == 1
    total = residual_alpha * packet_ref[:, : 2 * half].astype(jnp.float32)
    for ref in refs[:count]:
        total = total + ref[...].astype(jnp.float32)
    mean = jnp.mean(total, axis=1, keepdims=True)
    variance = jnp.mean(total * total, axis=1, keepdims=True) - mean * mean
    scaled = (total - mean) * lax.rsqrt(variance + norm_eps)
    left, right = scaled[:, :half], scaled[:, half:]
    own = jnp.where(flipped, right, left)
    far = jnp.where(flipped, left, right)
    own_ref[...] = (own * own_norm_ref[:1] + own_norm_ref[1:]).astype(jnp.bfloat16)
    far_ref[...] = (far * far_norm_ref[:1] + far_norm_ref[1:]).astype(jnp.bfloat16)


def place_kernel(core_ref, own_ref, far_ref, out_ref):
    rows = own_ref.shape[0]
    flipped = core_ref[0] == 1
    own, far = own_ref[...], far_ref[...]
    out_ref[:rows, :] = jnp.where(flipped, far, own)
    out_ref[rows:, :] = jnp.where(flipped, own, far)


def routed_kernel(width, experts, local, place_ref, first_ref, second_ref, branch_ref, *refs):
    held, outs = refs[:9], refs[9:11]
    own_expert, core = place_ref[0], place_ref[1]
    rows = jnp.concatenate([first_ref[...], second_ref[...]], axis=0)
    block = first_ref.shape[0]
    tokens = rows[:, :width]
    spread = rows[:, width:].astype(jnp.float32)
    lane = lax.broadcasted_iota(jnp.int32, spread.shape, 1)
    shares = []
    for index in range(local):
        chosen = (lane == own_expert + index) | (lane == own_expert + index + experts)
        shares.append(jnp.sum(jnp.where(chosen, spread, 0.0), axis=1, keepdims=True))
    logit = jnp.sum(
        tokens.astype(jnp.float32) * branch_ref[...].astype(jnp.float32), axis=1, keepdims=True
    )
    hidden = []
    for side in range(2):
        for index in range(local):
            gate_part = product(tokens, held[2 * side][index])
            up_part = product(tokens, held[2 * side + 1][index])
            piece = jax.nn.silu(gate_part) * up_part * shares[index]
            hidden.append((piece.astype(jnp.bfloat16), held[4 + side], index))
    dense_part = lax.dot_general(
        tokens, held[6][...], (((1,), (1,)), ((), ())), preferred_element_type=jnp.float32
    )
    dense_hidden = (jax.nn.gelu(dense_part) * jax.nn.sigmoid(logit)).astype(jnp.bfloat16)
    part = width // 2
    for side in range(2):
        own_side = core == side
        columns = jnp.where(own_side, held[7][...], held[8][...])
        for start in range(0, part, min(part, 512)):
            stop = min(start + 512, part)
            total = product(dense_hidden, columns[:, start:stop])
            low, high = side * part + start, side * part + stop
            for piece, down, index in hidden:
                total = total + product(piece, down[index, :, low:high])
            rounded = total.astype(jnp.bfloat16)
            outs[0][:, low:high] = rounded[:block]
            outs[1][:, low:high] = rounded[block:]


def routed_rows(width, place, first, second, branch_gate, experts, weights):
    rows = first.shape[0]
    return pl.pallas_call(
        functools.partial(routed_kernel, width, experts, weights[0].shape[0]),
        out_shape=[jax.ShapeDtypeStruct((rows, width), jnp.bfloat16)] * 2,
        in_specs=[smem, vmem, vmem, vmem] + [vmem] * len(weights),
        out_specs=[vmem] * 2,
        compiler_params=params(16),
        cost_estimate=cost(24 * rows * weights[0].size, 8 << 20),
        name="routed_rows",
    )(place, first, second, branch_gate[None, :], *weights)


def body(
    layer_input,
    ssm_state,
    w_input,
    decay_rate,
    frequency,
    step_log,
    input_map,
    output_map,
    skip_gain,
    glu_weight,
    mix_out,
    norm_gain,
    norm_shift,
    route_ids,
    route_weights,
    gate_expert,
    up_expert,
    down_expert,
    gate_shared,
    up_shared,
    down_shared,
    dense_in,
    dense_out,
    branch_gate,
    final_gain,
    final_shift,
):
    count_ep = lax.axis_size("ep")
    count_tp = lax.axis_size("tp")
    core = lax.axis_index("tp")
    rank = lax.axis_index("ep")
    outer, inner = split_of(count_ep)
    seq_rows, width = layer_input.shape
    local_experts = gate_expert.shape[0]
    experts = local_experts * count_ep
    place = jnp.stack([rank * local_experts, core]).astype(jnp.int32)
    core_word = core.astype(jnp.int32)[None]

    def swapped(value):
        return lax.ppermute(value, "tp", [(t, 1 - t) for t in range(count_tp)])

    def moved(value, moves):
        return lax.ppermute(value, both_axes, moves)

    norm_own = jnp.stack([final_gain, final_shift])
    gate_far = swapped(gate_expert)
    up_far = swapped(up_expert)
    down_far = swapped(down_expert)
    dense_far = swapped(dense_out)
    norm_far = swapped(norm_own)
    core_rows = seq_rows // count_tp
    state_rows = ssm_state.reshape(-1, ssm_state.shape[3])
    half_channels = jax.ShapeDtypeStruct((core_rows, w_input.shape[1]), jnp.bfloat16)
    sources = [
        step_log[None, :],
        decay_rate,
        frequency,
        layer_input,
        w_input,
        jnp.swapaxes(input_map, 2, 3),
        state_rows,
        output_map,
        skip_gain,
    ]
    activated, far_tokens, new_rows = pl.pallas_call(
        mixer_kernel,
        out_shape=[
            half_channels,
            half_channels,
            jax.ShapeDtypeStruct(state_rows.shape, jnp.float32),
        ],
        in_specs=[smem] + [in_hbm] * len(sources),
        out_specs=[vmem] * 3,
        scratch_shapes=[pltpu.VMEM(value.shape, value.dtype) for value in sources]
        + [pltpu.SemaphoreType.DMA((len(sources),))],
        compiler_params=params(63),
        cost_estimate=cost(4 * seq_rows * w_input.size, 5 << 20),
        name="mixer",
    )(core_word, *sources)
    new_state = new_rows.reshape(ssm_state.shape)
    activated_far = swapped(far_tokens)
    packet_width = width + -(-2 * experts // 128) * 128
    packet_shape = jax.ShapeDtypeStruct((core_rows, packet_width), jnp.bfloat16)
    row_shape = jax.ShapeDtypeStruct((core_rows, width), jnp.bfloat16)
    packet = pl.pallas_call(
        functools.partial(mix_kernel, experts),
        out_shape=packet_shape,
        in_specs=[smem] + [vmem] * 9,
        out_specs=vmem,
        compiler_params=params(12),
        cost_estimate=cost(2 * seq_rows * (glu_weight.size + mix_out.size), 3 << 20),
        name="mix",
    )(
        core_word,
        activated,
        activated_far,
        glu_weight,
        mix_out,
        layer_input,
        norm_gain[None, :],
        norm_shift[None, :],
        route_ids,
        route_weights,
    )
    packet_far = swapped(packet)
    line = [packet]
    for step in range(1, outer):
        line.append(moved(packet, line_moves(step, count_ep, count_tp)))
    line = pl.pallas_call(
        join_kernel,
        out_shape=jax.ShapeDtypeStruct((outer * core_rows, packet_width), jnp.bfloat16),
        in_specs=[vmem] * outer,
        out_specs=vmem,
        compiler_params=params(12),
        cost_estimate=cost(outer * core_rows * packet_width, 1 << 20),
        name="join",
    )(*line)
    arrived = [line]
    for step in range(1, inner):
        arrived.append(moved(line, plane_moves(step, count_ep, count_tp)))
    gate_held, up_held, down_held, dense_held = loaded([gate_far, up_far, down_far, dense_far])
    weights = [gate_expert, up_expert, gate_held, up_held, down_expert, down_held]
    weights += [dense_in, dense_out, dense_held]
    results = {}
    steps = [*range(1, inner), 0]
    for slot in range(inner // 2):
        pair = steps[2 * slot : 2 * slot + 2]
        first, second = (arrived[step] for step in pair)
        done = routed_rows(width, place, first, second, branch_gate, experts, weights)
        results.update(zip(pair, done))
    parts = [results[0]]
    for step in range(1, inner):
        moves = backward(plane_moves(step, count_ep, count_tp))
        parts.append(moved(results[step], moves))
    held = (gate_shared, up_shared, down_shared)
    shared, shared_sent = pl.pallas_call(
        shared_kernel,
        out_shape=[row_shape] * 2,
        in_specs=[vmem] * 2 + [in_hbm] * 3,
        out_specs=[vmem] * 2,
        scratch_shapes=[pltpu.VMEM(value.shape, value.dtype) for value in held]
        + [pltpu.SemaphoreType.DMA((3,))],
        compiler_params=params(12),
        cost_estimate=cost(6 * seq_rows * gate_shared.size, 3 << 20),
        name="shared_mlp",
    )(packet, packet_far, *held)
    shared_far = swapped(shared_sent)
    blocks = pl.pallas_call(
        functools.partial(sum_kernel, inner),
        out_shape=[row_shape] * outer,
        in_specs=[vmem] * inner,
        out_specs=[vmem] * outer,
        compiler_params=params(12),
        cost_estimate=cost(inner * outer * core_rows * width, 3 << 20),
        name="total",
    )(*parts)
    terms = [blocks[0]]
    for step in range(1, outer):
        moves = backward(line_moves(step, count_ep, count_tp))
        terms.append(moved(blocks[step], moves))
    half_shape = jax.ShapeDtypeStruct((core_rows, width // count_tp), jnp.bfloat16)
    terms += [shared, shared_far]
    own_half, far_half = pl.pallas_call(
        functools.partial(final_kernel, len(terms)),
        out_shape=[half_shape] * 2,
        in_specs=[smem] + [vmem] * (3 + len(terms)),
        out_specs=[vmem] * 2,
        compiler_params=params(12),
        cost_estimate=cost(10 * core_rows * width, 1 << 20),
        name="final",
    )(core_word, packet, norm_own, norm_far, *terms)
    handed = swapped(far_half)
    layer_output = pl.pallas_call(
        place_kernel,
        out_shape=jax.ShapeDtypeStruct((seq_rows, width // count_tp), jnp.bfloat16),
        in_specs=[smem, vmem, vmem],
        out_specs=vmem,
        compiler_params=params(12),
        cost_estimate=cost(seq_rows * width, 1 << 18),
        name="place",
    )(core_word, own_half, handed)
    return (layer_output, new_state)


def solution(mesh):
    placed = (
        P(("grp", "ep"), None),
        P(None, ("grp", "ep"), "tp", None),
        P(None, "tp"),
        P("tp", None),
        P("tp", None),
        P("tp"),
        P(None, "tp", None, None),
        P(None, "tp", None, None),
        P("tp", None),
        P(),
        P(),
        P(),
        P(),
        P(("grp", "ep"), None),
        P(("grp", "ep"), None),
        P("ep", None, "tp"),
        P("ep", None, "tp"),
        P("ep", "tp", None),
        P(None, "tp"),
        P(None, "tp"),
        P("tp", None),
        P("ep", None),
        P("ep", "tp"),
        P(),
        P("tp"),
        P("tp"),
    )
    return jax.shard_map(
        body,
        mesh=mesh,
        in_specs=placed,
        out_specs=(P(("grp", "ep"), "tp"), P(None, ("grp", "ep"), "tp", None)),
        check_vma=False,
    )
```

```python
import functools

import jax
import jax.numpy as jnp
from jax import lax
from jax.experimental import pallas as pl
from jax.experimental.pallas import tpu as pltpu
from jax.sharding import PartitionSpec as P


residual_alpha = 1.681792830507429
route_scale = 2.5
norm_eps = 1e-05
both_axes = ("ep", "tp")


def split_of(count_ep):
    inner = 1
    while inner < 4 and count_ep % (inner * 2) == 0:
        inner *= 2
    return (count_ep // inner, inner)


def outer_peer(place, step, outer):
    return place ^ step if outer & (outer - 1) == 0 else (place + step) % outer


def line_moves(step, count_ep, count_tp):
    outer, inner = split_of(count_ep)
    moves = []
    for rank in range(count_ep):
        peer = outer_peer(rank // inner, step, outer) * inner + rank % inner
        moves += [(rank * count_tp + t, peer * count_tp + t) for t in range(count_tp)]
    return moves


def plane_moves(step, count_ep, count_tp):
    inner = split_of(count_ep)[1]
    moves = []
    for rank in range(count_ep):
        for t in range(count_tp):
            crossed = inner == 4 and step < 3 and t % 2 == 1
            peer = rank ^ (3 - step if crossed else step)
            moves.append((rank * count_tp + t, peer * count_tp + t))
    return moves


def backward(moves):
    return [(target, source) for source, target in moves]


vmem = pl.BlockSpec(memory_space=pltpu.VMEM)
smem = pl.BlockSpec(memory_space=pltpu.SMEM)
in_hbm = pl.BlockSpec(memory_space=pltpu.HBM)


def product(left, right):
    return jnp.dot(left, right, preferred_element_type=jnp.float32)


def params(mebibytes):
    return pltpu.CompilerParams(vmem_limit_bytes=mebibytes << 20)


def cost(flops, moved):
    return pl.CostEstimate(flops=flops, bytes_accessed=moved, transcendentals=0)


def token_half(ref, flipped):
    half = ref.shape[0] // 2
    return jnp.where(flipped, ref[half:, :], ref[:half, :])


def halves(value):
    high = value.astype(jnp.bfloat16)
    return high, (value - high.astype(jnp.float32)).astype(jnp.bfloat16)


def mixer_kernel(core_ref, *refs):
    sources, (own_ref, far_ref, new_ref) = refs[:9], refs[9:12]
    held, sems = refs[12:21], refs[21]
    copies = []
    for index, (source, target) in enumerate(zip(sources, held)):
        copies.append(pltpu.make_async_copy(source, target, sems.at[index]))
        copies[-1].start()
    step_ref, rate_ref, frequency_ref, input_ref, project_ref, drive_ref, state_ref, readout_ref, skip_ref = held
    rows = input_ref.shape[0]
    groups, _ = rate_ref.shape
    channels = skip_ref.shape[1]
    for copy in copies[:3]:
        copy.wait()
    square = lax.broadcasted_iota(jnp.int32, (groups, groups), 0) == lax.broadcasted_iota(
        jnp.int32, (groups, groups), 1
    )
    step_size = jnp.exp(jnp.sum(jnp.where(square, step_ref[...], 0.0), axis=1, keepdims=True))
    rate, frequency = rate_ref[...], frequency_ref[...]
    magnitude = jnp.exp(-rate * step_size)
    rotation = frequency * step_size
    decay_re = magnitude * jnp.cos(rotation)
    decay_im = magnitude * jnp.sin(rotation)
    denominator = rate * rate + frequency * frequency
    factor_re = (decay_im * frequency - (decay_re - 1.0) * rate) / denominator
    factor_im = (-decay_im * rate - (decay_re - 1.0) * frequency) / denominator
    for copy in copies[3:]:
        copy.wait()
    flipped = core_ref[0] == 1
    projected = product(input_ref[...], project_ref[...]).astype(jnp.bfloat16)
    responses = []
    for index in range(groups):
        one = slice(index, index + 1)
        inputs = projected[:, index * channels : (index + 1) * channels]
        twice = jnp.concatenate([inputs, inputs], axis=1)
        map_re, map_im = drive_ref[0, index], drive_ref[1, index]
        drive_re = halves(factor_re[one] * map_re - factor_im[one] * map_im)
        drive_im = halves(factor_re[one] * map_im + factor_im[one] * map_re)
        old_re = state_ref[pl.ds(index, rows, groups), :]
        old_im = state_ref[pl.ds(rows * groups + index, rows, groups), :]
        new_re = decay_re[one] * old_re - decay_im[one] * old_im
        new_im = decay_re[one] * old_im + decay_im[one] * old_re
        new_re = new_re + product(twice, jnp.concatenate(drive_re, axis=0))
        new_im = new_im + product(twice, jnp.concatenate(drive_im, axis=0))
        new_ref[pl.ds(index, rows, groups), :] = new_re
        new_ref[pl.ds(rows * groups + index, rows, groups), :] = new_im
        high, low = halves(jnp.concatenate([new_re, new_im], axis=1))
        readout = jnp.concatenate([readout_ref[0, index], -readout_ref[1, index]], axis=1)
        read_high, read_low = halves(readout)
        response = lax.dot_general(
            jnp.concatenate([high, low, high], axis=1),
            jnp.concatenate([read_high, read_high, read_low], axis=1),
            (((1,), (1,)), ((), ())),
            preferred_element_type=jnp.float32,
        )
        responses.append(response + skip_ref[one, :] * inputs.astype(jnp.float32))
    activated = jax.nn.gelu(jnp.concatenate(responses, axis=1)).astype(jnp.bfloat16)
    own_ref[...] = jnp.where(flipped, activated[rows // 2 :], activated[: rows // 2])
    far_ref[...] = jnp.where(flipped, activated[: rows // 2], activated[rows // 2 :])


def load_kernel(count, *refs):
    sems = refs[2 * count]
    copies = []
    for index in range(count):
        copies.append(pltpu.make_async_copy(refs[index], refs[count + index], sems.at[index]))
        copies[-1].start()
    for copy in copies:
        copy.wait()


def loaded(values):
    return pl.pallas_call(
        functools.partial(load_kernel, len(values)),
        out_shape=[jax.ShapeDtypeStruct(value.shape, value.dtype) for value in values],
        in_specs=[in_hbm] * len(values),
        out_specs=[vmem] * len(values),
        scratch_shapes=[pltpu.SemaphoreType.DMA((len(values),))],
        compiler_params=params(12),
        cost_estimate=cost(1 << 22, 8 << 20),
        name="load",
    )(*values)


def mix_kernel(
    experts,
    core_ref,
    own_ref,
    far_ref,
    glu_ref,
    mix_ref,
    input_ref,
    gain_ref,
    shift_ref,
    ids_ref,
    scores_ref,
    packet_ref,
):
    width = input_ref.shape[1]
    flipped = core_ref[0] == 1
    own, far = own_ref[...], far_ref[...]
    every = jnp.concatenate([jnp.where(flipped, far, own), jnp.where(flipped, own, far)], axis=1)
    gated = (every.astype(jnp.float32) * jax.nn.sigmoid(product(every, glu_ref[...]))).astype(
        jnp.bfloat16
    )
    mixed = product(gated, mix_ref[...]).astype(jnp.bfloat16).astype(jnp.float32)
    values = residual_alpha * token_half(input_ref, flipped).astype(jnp.float32) + mixed
    mean = jnp.mean(values, axis=1, keepdims=True)
    centered = values - mean
    variance = jnp.mean(centered * centered, axis=1, keepdims=True)
    normed = centered * lax.rsqrt(variance + norm_eps) * gain_ref[...] + shift_ref[...]
    packet_ref[:, :width] = normed.astype(jnp.bfloat16)
    scores = token_half(scores_ref, flipped)
    ids = token_half(ids_ref, flipped)
    weights = scores / jnp.sum(scores, axis=1, keepdims=True) * route_scale
    rows, extra = packet_ref.shape[0], packet_ref.shape[1] - width
    lane = lax.broadcasted_iota(jnp.int32, (rows, extra), 1)
    expert = jnp.where(lane < experts, lane, lane - experts)
    spread = jnp.zeros((rows, extra), jnp.float32)
    for choice in range(scores.shape[1]):
        named = ids[:, choice : choice + 1] == expert
        spread = spread + jnp.where(named, weights[:, choice : choice + 1], 0.0)
    high = spread.astype(jnp.bfloat16).astype(jnp.float32)
    packet_ref[:, width:] = jnp.where(lane < experts, high, spread - high).astype(jnp.bfloat16)


def shared_kernel(own_ref, far_ref, gate_hbm, up_hbm, down_hbm, own_out, far_out, *scratch):
    gate_ref, up_ref, down_ref, sems = scratch
    copies = []
    for index, (source, target) in enumerate(zip((gate_hbm, up_hbm, down_hbm), scratch)):
        copies.append(pltpu.make_async_copy(source, target, sems.at[index]))
        copies[-1].start()
    width, half = own_out.shape[1], own_out.shape[0]
    normed = jnp.concatenate([own_ref[:, :width], far_ref[:, :width]], axis=0)
    copies[0].wait()
    gate_part = product(normed, gate_ref[...])
    copies[1].wait()
    hidden = (jax.nn.silu(gate_part) * product(normed, up_ref[...])).astype(jnp.bfloat16)
    copies[2].wait()
    result = product(hidden, down_ref[...]).astype(jnp.bfloat16)
    own_out[...] = result[:half]
    far_out[...] = result[half:]


def join_kernel(*refs):
    rows = refs[0].shape[0]
    for place, ref in enumerate(refs[:-1]):
        refs[-1][place * rows : (place + 1) * rows, :] = ref[...]


def sum_kernel(count, *refs):
    rows = refs[count].shape[0]
    for place, out_ref in enumerate(refs[count:]):
        total = refs[0][place * rows : (place + 1) * rows, :].astype(jnp.float32)
        for ref in refs[1:count]:
            total = total + ref[place * rows : (place + 1) * rows, :].astype(jnp.float32)
        out_ref[...] = total.astype(jnp.bfloat16)


def final_kernel(count, core_ref, packet_ref, own_norm_ref, far_norm_ref, *refs):
    own_ref, far_ref = refs[count:]
    half = own_ref.shape[1]
    flipped = core_ref[0] == 1
    total = residual_alpha * packet_ref[:, : 2 * half].astype(jnp.float32)
    for ref in refs[:count]:
        total = total + ref[...].astype(jnp.float32)
    mean = jnp.mean(total, axis=1, keepdims=True)
    variance = jnp.mean(total * total, axis=1, keepdims=True) - mean * mean
    scaled = (total - mean) * lax.rsqrt(variance + norm_eps)
    left, right = scaled[:, :half], scaled[:, half:]
    own = jnp.where(flipped, right, left)
    far = jnp.where(flipped, left, right)
    own_ref[...] = (own * own_norm_ref[:1] + own_norm_ref[1:]).astype(jnp.bfloat16)
    far_ref[...] = (far * far_norm_ref[:1] + far_norm_ref[1:]).astype(jnp.bfloat16)


def place_kernel(core_ref, own_ref, far_ref, out_ref):
    rows = own_ref.shape[0]
    flipped = core_ref[0] == 1
    own, far = own_ref[...], far_ref[...]
    out_ref[:rows, :] = jnp.where(flipped, far, own)
    out_ref[rows:, :] = jnp.where(flipped, own, far)


def routed_kernel(width, experts, local, place_ref, first_ref, second_ref, branch_ref, *refs):
    held, outs = refs[:9], refs[9:11]
    own_expert, core = place_ref[0], place_ref[1]
    rows = jnp.concatenate([first_ref[...], second_ref[...]], axis=0)
    block = first_ref.shape[0]
    tokens = rows[:, :width]
    spread = rows[:, width:].astype(jnp.float32)
    lane = lax.broadcasted_iota(jnp.int32, spread.shape, 1)
    shares = []
    for index in range(local):
        chosen = (lane == own_expert + index) | (lane == own_expert + index + experts)
        shares.append(jnp.sum(jnp.where(chosen, spread, 0.0), axis=1, keepdims=True))
    logit = jnp.sum(
        tokens.astype(jnp.float32) * branch_ref[...].astype(jnp.float32), axis=1, keepdims=True
    )
    hidden = []
    for side in range(2):
        for index in range(local):
            gate_part = product(tokens, held[2 * side][index])
            up_part = product(tokens, held[2 * side + 1][index])
            piece = jax.nn.silu(gate_part) * up_part * shares[index]
            hidden.append((piece.astype(jnp.bfloat16), held[4 + side], index))
    dense_part = lax.dot_general(
        tokens, held[6][...], (((1,), (1,)), ((), ())), preferred_element_type=jnp.float32
    )
    dense_hidden = (jax.nn.gelu(dense_part) * jax.nn.sigmoid(logit)).astype(jnp.bfloat16)
    part = width // 2
    for side in range(2):
        own_side = core == side
        columns = jnp.where(own_side, held[7][...], held[8][...])
        for start in range(0, part, min(part, 512)):
            stop = min(start + 512, part)
            total = product(dense_hidden, columns[:, start:stop])
            low, high = side * part + start, side * part + stop
            for piece, down, index in hidden:
                total = total + product(piece, down[index, :, low:high])
            rounded = total.astype(jnp.bfloat16)
            outs[0][:, low:high] = rounded[:block]
            outs[1][:, low:high] = rounded[block:]


def routed_rows(width, place, first, second, branch_gate, experts, weights):
    rows = first.shape[0]
    return pl.pallas_call(
        functools.partial(routed_kernel, width, experts, weights[0].shape[0]),
        out_shape=[jax.ShapeDtypeStruct((rows, width), jnp.bfloat16)] * 2,
        in_specs=[smem, vmem, vmem, vmem] + [vmem] * len(weights),
        out_specs=[vmem] * 2,
        compiler_params=params(16),
        cost_estimate=cost(24 * rows * weights[0].size, 8 << 20),
        name="routed_rows",
    )(place, first, second, branch_gate[None, :], *weights)


def body(
    layer_input,
    ssm_state,
    w_input,
    decay_rate,
    frequency,
    step_log,
    input_map,
    output_map,
    skip_gain,
    glu_weight,
    mix_out,
    norm_gain,
    norm_shift,
    route_ids,
    route_weights,
    gate_expert,
    up_expert,
    down_expert,
    gate_shared,
    up_shared,
    down_shared,
    dense_in,
    dense_out,
    branch_gate,
    final_gain,
    final_shift,
):
    count_ep = lax.axis_size("ep")
    count_tp = lax.axis_size("tp")
    core = lax.axis_index("tp")
    rank = lax.axis_index("ep")
    outer, inner = split_of(count_ep)
    seq_rows, width = layer_input.shape
    local_experts = gate_expert.shape[0]
    experts = local_experts * count_ep
    place = jnp.stack([rank * local_experts, core]).astype(jnp.int32)
    core_word = core.astype(jnp.int32)[None]

    def swapped(value):
        return lax.ppermute(value, "tp", [(t, 1 - t) for t in range(count_tp)])

    def moved(value, moves):
        return lax.ppermute(value, both_axes, moves)

    norm_own = jnp.stack([final_gain, final_shift])
    gate_far = swapped(gate_expert)
    up_far = swapped(up_expert)
    down_far = swapped(down_expert)
    dense_far = swapped(dense_out)
    norm_far = swapped(norm_own)
    core_rows = seq_rows // count_tp
    state_rows = ssm_state.reshape(-1, ssm_state.shape[3])
    half_channels = jax.ShapeDtypeStruct((core_rows, w_input.shape[1]), jnp.bfloat16)
    sources = [
        step_log[None, :],
        decay_rate,
        frequency,
        layer_input,
        w_input,
        jnp.swapaxes(input_map, 2, 3),
        state_rows,
        output_map,
        skip_gain,
    ]
    activated, far_tokens, new_rows = pl.pallas_call(
        mixer_kernel,
        out_shape=[
            half_channels,
            half_channels,
            jax.ShapeDtypeStruct(state_rows.shape, jnp.float32),
        ],
        in_specs=[smem] + [in_hbm] * len(sources),
        out_specs=[vmem] * 3,
        scratch_shapes=[pltpu.VMEM(value.shape, value.dtype) for value in sources]
        + [pltpu.SemaphoreType.DMA((len(sources),))],
        compiler_params=params(63),
        cost_estimate=cost(4 * seq_rows * w_input.size, 5 << 20),
        name="mixer",
    )(core_word, *sources)
    new_state = new_rows.reshape(ssm_state.shape)
    activated_far = swapped(far_tokens)
    packet_width = width + -(-2 * experts // 128) * 128
    packet_shape = jax.ShapeDtypeStruct((core_rows, packet_width), jnp.bfloat16)
    row_shape = jax.ShapeDtypeStruct((core_rows, width), jnp.bfloat16)
    packet = pl.pallas_call(
        functools.partial(mix_kernel, experts),
        out_shape=packet_shape,
        in_specs=[smem] + [vmem] * 9,
        out_specs=vmem,
        compiler_params=params(12),
        cost_estimate=cost(2 * seq_rows * (glu_weight.size + mix_out.size), 3 << 20),
        name="mix",
    )(
        core_word,
        activated,
        activated_far,
        glu_weight,
        mix_out,
        layer_input,
        norm_gain[None, :],
        norm_shift[None, :],
        route_ids,
        route_weights,
    )
    packet_far = swapped(packet)
    line = [packet]
    for step in range(1, outer):
        line.append(moved(packet, line_moves(step, count_ep, count_tp)))
    line = pl.pallas_call(
        join_kernel,
        out_shape=jax.ShapeDtypeStruct((outer * core_rows, packet_width), jnp.bfloat16),
        in_specs=[vmem] * outer,
        out_specs=vmem,
        compiler_params=params(12),
        cost_estimate=cost(outer * core_rows * packet_width, 1 << 20),
        name="join",
    )(*line)
    arrived = [line]
    for step in range(1, inner):
        arrived.append(moved(line, plane_moves(step, count_ep, count_tp)))
    gate_held, up_held, down_held, dense_held = loaded([gate_far, up_far, down_far, dense_far])
    weights = [gate_expert, up_expert, gate_held, up_held, down_expert, down_held]
    weights += [dense_in, dense_out, dense_held]
    results = {}
    steps = [*range(1, inner), 0]
    for slot in range(inner // 2):
        pair = steps[2 * slot : 2 * slot + 2]
        first, second = (arrived[step] for step in pair)
        done = routed_rows(width, place, first, second, branch_gate, experts, weights)
        results.update(zip(pair, done))
    parts = [results[0]]
    for step in range(1, inner):
        moves = backward(plane_moves(step, count_ep, count_tp))
        parts.append(moved(results[step], moves))
    held = (gate_shared, up_shared, down_shared)
    shared, shared_sent = pl.pallas_call(
        shared_kernel,
        out_shape=[row_shape] * 2,
        in_specs=[vmem] * 2 + [in_hbm] * 3,
        out_specs=[vmem] * 2,
        scratch_shapes=[pltpu.VMEM(value.shape, value.dtype) for value in held]
        + [pltpu.SemaphoreType.DMA((3,))],
        compiler_params=params(12),
        cost_estimate=cost(6 * seq_rows * gate_shared.size, 3 << 20),
        name="shared_mlp",
    )(packet, packet_far, *held)
    shared_far = swapped(shared_sent)
    blocks = pl.pallas_call(
        functools.partial(sum_kernel, inner),
        out_shape=[row_shape] * outer,
        in_specs=[vmem] * inner,
        out_specs=[vmem] * outer,
        compiler_params=params(12),
        cost_estimate=cost(inner * outer * core_rows * width, 3 << 20),
        name="total",
    )(*parts)
    terms = [blocks[0]]
    for step in range(1, outer):
        moves = backward(line_moves(step, count_ep, count_tp))
        terms.append(moved(blocks[step], moves))
    half_shape = jax.ShapeDtypeStruct((core_rows, width // count_tp), jnp.bfloat16)
    terms += [shared, shared_far]
    own_half, far_half = pl.pallas_call(
        functools.partial(final_kernel, len(terms)),
        out_shape=[half_shape] * 2,
        in_specs=[smem] + [vmem] * (3 + len(terms)),
        out_specs=[vmem] * 2,
        compiler_params=params(12),
        cost_estimate=cost(10 * core_rows * width, 1 << 20),
        name="final",
    )(core_word, packet, norm_own, norm_far, *terms)
    handed = swapped(far_half)
    layer_output = pl.pallas_call(
        place_kernel,
        out_shape=jax.ShapeDtypeStruct((seq_rows, width // count_tp), jnp.bfloat16),
        in_specs=[smem, vmem, vmem],
        out_specs=vmem,
        compiler_params=params(12),
        cost_estimate=cost(seq_rows * width, 1 << 18),
        name="place",
    )(core_word, own_half, handed)
    return (layer_output, new_state)


def solution(mesh):
    placed = (
        P(("grp", "ep"), None),
        P(None, ("grp", "ep"), "tp", None),
        P(None, "tp"),
        P("tp", None),
        P("tp", None),
        P("tp"),
        P(None, "tp", None, None),
        P(None, "tp", None, None),
        P("tp", None),
        P(),
        P(),
        P(),
        P(),
        P(("grp", "ep"), None),
        P(("grp", "ep"), None),
        P("ep", None, "tp"),
        P("ep", None, "tp"),
        P("ep", "tp", None),
        P(None, "tp"),
        P(None, "tp"),
        P("tp", None),
        P("ep", None),
        P("ep", "tp"),
        P(),
        P("tp"),
        P("tp"),
    )
    return jax.shard_map(
        body,
        mesh=mesh,
        in_specs=placed,
        out_specs=(P(("grp", "ep"), "tp"), P(None, ("grp", "ep"), "tp", None)),
        check_vma=False,
    )
```
